32 devices in a mesh: ep: 16 (over z, y, x), tp: 2 (over core).
Axes of the slice: x: 2, y: 2, z: 4, core: 2. Of those that a mesh axis runs over, the one named last changes fastest.
Arguments:
- tokens: bfloat16 [1024, 1024], P('ep', 'tp'), may hold values from -6 to 6
- norm_gain: float32 [1024], P('tp'), may hold values from 0.1 to 1.9
- routing: int32 [1024, 2], P('ep'), may hold values from 0 to 31, as said below
- route_weight: float32 [1024, 2], P('ep'), may hold values from 0.25 to 1
- w_gate: bfloat16 [32, 1024, 512], P('ep', None, 'tp'), may hold values from -0.1875 to 0.1875
- w_up: bfloat16 [32, 1024, 512], P('ep', None, 'tp'), may hold values from -0.1875 to 0.1875
- w_down: bfloat16 [32, 512, 1024], P('ep', None, 'tp'), may hold values from -0.25 to 0.25
Outputs:
- mixed: bfloat16 [1024, 1024], P('ep', 'tp')
The draws below stay inside these ranges and needn't reach their ends.
Inputs may be any that keep to these rules, and one draw needn't show every extreme that they name: `routing`: each row names 2 different experts, all in the same group of 8 consecutive expert numbers. Among the rows of one device (aligned blocks of 64 rows) no expert is named more than 8 times, and in every block some expert is named exactly 8 times.
All inputs are finite; a program needn't handle non-finite values.
Results may differ from the reference program's by a relative error of at most 0.0015.
Values may be sent and summed in bfloat16 or wider, within the bound.
A program may use at most 64 MiB of HBM per device.

```python
import jax
import jax.numpy as jnp
from jax import lax

D = 1024
FFE = 512
TOP_K = 2
GROUP_EXP = 8
EXP_DEV = 2
CAP = 8
TOK_DEV = 64
EXPERTS = 32
TOKENS = 1024


def route_table(key):
    blocks = TOKENS // TOK_DEV
    groups = EXPERTS // GROUP_EXP
    semi_cluster = GROUP_EXP // 2
    opening_tally = EXPERTS // 2
    cell_count = TOK_DEV // CAP
    pop_key = jax.random.fold_in(key, 11)
    group_scores = jax.random.randint(pop_key, (groups,), 0, 1 << 20) * groups + jnp.arange(groups)
    ranking = jnp.argsort(jnp.argsort(group_scores))
    favoured_specialist = ranking < max(1, groups // 4)
    extra_cluster = jnp.where(favoured_specialist, 400, 0)
    base_key = jax.random.fold_in(key, 23)

    def one_block(block_id):
        block_key = jax.random.fold_in(base_key, block_id)
        perm_key, rating_seed, seat_key, flip_key = jax.random.split(block_key, 4)
        raw = jax.random.randint(perm_key, (groups, GROUP_EXP), 0, 1 << 20) * GROUP_EXP + jnp.arange(GROUP_EXP)[None, :]
        local_perm = jnp.argsort(raw, axis=1)
        pair_table = (jnp.arange(groups)[:, None] * GROUP_EXP + local_perm).reshape(opening_tally, 2)
        position = jnp.argsort(pair_table.reshape(-1))
        slot_of = position // 2
        forward = (block_id + blocks // 2) % blocks * EXP_DEV
        previous = (block_id + blocks - 1) % blocks * EXP_DEV
        opening_labels = jnp.arange(opening_tally)
        affinity_grades = jax.random.randint(rating_seed, (opening_tally,), 0, 1024) + extra_cluster[opening_labels // semi_cluster]
        affinity_grades = affinity_grades + 8192 * (opening_labels == slot_of[forward]) + 8192 * (opening_labels == slot_of[previous])
        affinity_grades = affinity_grades * opening_tally + opening_labels
        unused, chosen = lax.top_k(affinity_grades, cell_count)
        seating = jax.random.permutation(seat_key, TOK_DEV)
        cell_of = seating // CAP
        pair_ids = pair_table[chosen[cell_of]]
        flipped = jax.random.randint(flip_key, (TOK_DEV,), 0, 2)
        first_pick = jnp.where(flipped == 1, pair_ids[:, 1], pair_ids[:, 0])
        second_pick = jnp.where(flipped == 1, pair_ids[:, 0], pair_ids[:, 1])
        return jnp.stack([first_pick, second_pick], axis=1)
    table = jax.vmap(one_block)(jnp.arange(blocks))
    return table.reshape(TOKENS, 2)


def draw_routing(key, part):
    return route_table(key).astype(jnp.int32)


def block_levels(key, shape, pieces, low, top_value):
    loudness, own = 1.0, jax.random.fold_in(key, 6)
    for dim, blocks in pieces:
        steps = jnp.exp(jax.random.uniform(jax.random.fold_in(own, dim), (blocks,), jnp.float32, low / len(pieces), top_value / len(pieces)))
        loudness = loudness * jnp.repeat(steps, shape[dim] // blocks).reshape([-1 if axis == dim else 1 for axis in range(len(shape))])
    return loudness


def scatter_about(stream_key, extent, width, reach, pieces=(), kind=jnp.bfloat16):
    loudness = block_levels(stream_key, extent, pieces, -0.22, 0.18) if pieces else 1.0
    array = jax.random.normal(stream_key, extent, jnp.float32) * width * loudness
    return jnp.minimum(jnp.maximum(array, -reach), reach).astype(kind)


def setup_inputs(seed: int = 0) -> dict:
    key_of = jax.random.split(jax.random.key(seed), 8)
    return {
        "tokens": scatter_about(key_of[0], (TOKENS, D), 1.0, 6.0, ((0, 16), (1, 2))),
        "norm_gain": jnp.clip(1.0 + 0.18 * jax.random.normal(key_of[1], (D,), jnp.float32), 0.1, 1.9),
        "routing": draw_routing(jax.random.fold_in(key_of[7], 71), 0),
        "route_weight": jnp.clip(0.25 + 0.75 * jax.random.uniform(key_of[3], (TOKENS, TOP_K), jnp.float32) ** block_levels(key_of[3], (TOKENS, TOP_K), ((0, 16),), -0.2, 0.2), 0.25, 1.0),
        "w_gate": scatter_about(key_of[4], (EXPERTS, D, FFE), D ** -0.5, 0.1875, ((0, 16), (2, 2))),
        "w_up": scatter_about(key_of[5], (EXPERTS, D, FFE), D ** -0.5, 0.1875, ((0, 16), (2, 2))),
        "w_down": scatter_about(key_of[6], (EXPERTS, FFE, D), FFE ** -0.5, 0.25, ((0, 16), (2, 2))),
    }


epsilon = 1e-06

def reference(tokens, norm_gain, routing, route_weight, w_gate, w_up, w_down):
    row_span = 32
    float_rows = tokens.astype(jnp.float32)
    scale = lax.rsqrt(lax.optimization_barrier(jnp.mean(float_rows * float_rows, axis=1, keepdims=True)) + epsilon)
    normed = (float_rows * scale * norm_gain[None, :]).astype(jnp.bfloat16)
    count = TOKENS * TOP_K
    flat_expert = routing.reshape(-1).astype(jnp.int32)
    flat_token = (jnp.arange(count) // TOP_K).astype(jnp.int32)
    flat_weight = route_weight.reshape(-1)
    sorting = jnp.argsort(flat_expert, stable=True).astype(jnp.int32)
    sorted_expert = flat_expert[sorting]
    counts = jnp.zeros((EXPERTS,), jnp.int32).at[flat_expert].add(1)
    starts = (jnp.cumsum(counts) - counts).astype(jnp.int32)
    padded = ((counts + row_span - 1) // row_span * row_span).astype(jnp.int32)
    pad_end = jnp.cumsum(padded).astype(jnp.int32)
    pad_start = (pad_end - padded).astype(jnp.int32)
    target = (pad_start[sorted_expert] + jnp.arange(count).astype(jnp.int32) - starts[sorted_expert]).astype(jnp.int32)
    block_count = -(-count // row_span) + EXPERTS
    row_total = block_count * row_span
    buffer = jnp.zeros((row_total, D), jnp.bfloat16).at[target].set(normed[flat_token[sorting]])
    block_expert = jnp.searchsorted(pad_end, (jnp.arange(block_count) * row_span).astype(jnp.int32), side='right')
    block_expert = jnp.minimum(block_expert.astype(jnp.int32), EXPERTS - 1).astype(jnp.int32)

    def run_block(inputs):
        block_rows, expert = inputs
        gate_acc = jnp.dot(block_rows, w_gate[expert], preferred_element_type=jnp.float32)
        up_acc = jnp.dot(block_rows, w_up[expert], preferred_element_type=jnp.float32)
        hidden = (jax.nn.silu(gate_acc) * up_acc).astype(jnp.bfloat16)
        return jnp.dot(hidden, w_down[expert], preferred_element_type=jnp.float32).astype(jnp.bfloat16)
    result = lax.map(run_block, (buffer.reshape(block_count, row_span, D), block_expert)).reshape(row_total, D)
    picked = result[target].astype(jnp.float32) * flat_weight[sorting][:, None]
    combined = jax.ops.segment_sum(picked, flat_token[sorting], num_segments=TOKENS)
    return combined.astype(jnp.bfloat16)
```

```python
import functools

import jax
import jax.numpy as jnp
from jax import lax
from jax.experimental import pallas as pl
from jax.experimental.pallas import tpu as pltpu
from jax.sharding import PartitionSpec as P

CAP = 8
EPSILON = 1e-06
MESH = pl.DeviceIdType.MESH


def each(count, body):
    if count <= 16:
        for k in range(1, count):
            body(k)
    else:
        lax.fori_loop(1, count, lambda k, c: (body(k), c)[1], 0)


def kernel(
    n, tok_ref, gain_ref, routing_ref, weight_ref, wg_hbm, wu_hbm, wd_hbm, out_ref,
    gains, wg, wu, wd, send_x, recv_x, send_y, recv_y,
    own_sem, far_send, far_recv, sx_sem, rx_sem, sy_sem, ry_sem,
):
    me, core = lax.axis_index("ep"), lax.axis_index("tp")
    other = 1 - core
    tokens, half = tok_ref.shape
    slots = 2 * n * CAP

    stores = ((wg_hbm, wg), (wu_hbm, wu), (wd_hbm, wd))
    own = [
        pltpu.make_async_copy(src.at[core], dst.at[core], own_sem.at[i])
        for i, (src, dst) in enumerate(stores)
    ]
    for copy in own:
        copy.start()

    barrier = pltpu.get_barrier_semaphore()

    def greet(k):
        peer = lax.rem(me + k, n)
        for c in range(2):
            pl.semaphore_signal(barrier, inc=1, device_id=(peer, c), device_id_type=MESH)

    pl.semaphore_signal(barrier, inc=1, device_id=(me, other), device_id_type=MESH)
    each(n, greet)

    gains[core] = gain_ref[...]
    experts = 2 * n
    names = lax.broadcasted_iota(jnp.int32, (tokens, experts), 1)
    picks = [routing_ref[:, k:k + 1] for k in range(2)]
    hot = [(picks[k] == names).astype(jnp.float32) for k in range(2)]
    row = lax.broadcasted_iota(jnp.int32, (tokens, tokens), 0)
    col = lax.broadcasted_iota(jnp.int32, (tokens, tokens), 1)
    before = (col < row).astype(jnp.bfloat16)
    earlier = jnp.dot(before, (hot[0] + hot[1]).astype(jnp.bfloat16), preferred_element_type=jnp.float32)
    places = lax.broadcasted_iota(jnp.int32, (tokens, slots), 1)
    chosen = []
    for k in range(2):
        rank = jnp.sum(earlier * hot[k], axis=1, keepdims=True).astype(jnp.int32)
        chosen.append(places == picks[k] * CAP + rank)
    spread = (chosen[0] | chosen[1]).astype(jnp.float32).astype(jnp.bfloat16)
    outgoing = lax.dot_general(
        spread, tok_ref[...], (((0,), (0,)), ((), ())), preferred_element_type=jnp.float32
    )
    send_x[...] = outgoing.reshape(2 * n, CAP, half).astype(jnp.bfloat16)

    pl.semaphore_wait(barrier, 2 * n - 1)

    def remote(src, dst, send, recv, peer, c):
        return pltpu.make_async_remote_copy(
            src_ref=src, dst_ref=dst, send_sem=send, recv_sem=recv,
            device_id=(peer, c), device_id_type=MESH,
        )

    def post(k):
        peer = lax.rem(me + k, n)
        for c in range(2):
            remote(send_x.at[peer * 2 + c], recv_x.at[core * n + me], sx_sem, rx_sem, peer, c).start()

    each(n, post)
    remote(send_x.at[me * 2 + other], recv_x.at[core * n + me], sx_sem, rx_sem, me, other).start()
    pltpu.make_async_copy(send_x.at[me * 2 + core], recv_x.at[core * n + me], rx_sem).start()
    far = [remote(gain_ref, gains.at[core], far_send.at[3], far_recv.at[3], me, other)] + [
        remote(src.at[other], dst.at[core], far_send.at[i], far_recv.at[i], me, other)
        for i, (src, dst) in enumerate(stores)
    ]
    for copy in far:
        copy.start()

    for copy in own:
        copy.wait()
    for copy in far:
        copy.wait()
    pltpu.make_async_copy(recv_x, recv_x, rx_sem).wait()

    rows = n * CAP
    parts = [recv_x[h * n:(h + 1) * n].astype(jnp.float32).reshape(rows, half) for h in range(2)]
    squares = sum(jnp.sum(p * p, axis=1, keepdims=True) for p in parts)
    scale = lax.rsqrt(squares / (2 * half) + EPSILON)
    normed = jnp.concatenate(
        [(p * scale * gains[h]).astype(jnp.bfloat16) for h, p in enumerate(parts)], axis=1
    )
    hidden = []
    for h in range(2):
        gate = jnp.dot(normed, wg[h], preferred_element_type=jnp.float32)
        up = jnp.dot(normed, wu[h], preferred_element_type=jnp.float32)
        hidden.append((jax.nn.silu(gate) * up).astype(jnp.bfloat16))
    hidden = jnp.concatenate(hidden, axis=1)
    for f in range(2):
        result = jnp.dot(hidden, wd[f], preferred_element_type=jnp.float32)
        send_y[f * n:(f + 1) * n] = result.reshape(n, CAP, half).astype(jnp.bfloat16)

    def reply(k):
        peer = lax.rem(me + k, n)
        for c in range(2):
            remote(send_y.at[c * n + peer], recv_y.at[me * 2 + core], sy_sem, ry_sem, peer, c).start()

    each(n, reply)
    remote(send_y.at[other * n + me], recv_y.at[me * 2 + core], sy_sem, ry_sem, me, other).start()
    pltpu.make_async_copy(send_y.at[core * n + me], recv_y.at[me * 2 + core], ry_sem).start()
    pltpu.make_async_copy(recv_y, recv_y, ry_sem).wait()

    back = recv_y[...].astype(jnp.float32).reshape(slots, half).astype(jnp.bfloat16)
    total = 0.0
    for k in range(2):
        pick = chosen[k].astype(jnp.float32).astype(jnp.bfloat16)
        total = total + weight_ref[:, k:k + 1] * jnp.dot(pick, back, preferred_element_type=jnp.float32)
    out_ref[...] = total.astype(jnp.bfloat16)
    sent = pl.ds(0, 2 * n - 1)
    pltpu.make_async_copy(send_x.at[sent], send_x.at[sent], sx_sem).wait()
    pltpu.make_async_copy(send_y.at[sent], send_y.at[sent], sy_sem).wait()


def solution(mesh):
    n = mesh.shape["ep"]

    def local(tokens, norm_gain, routing, route_weight, w_gate, w_up, w_down):
        rows, half = tokens.shape
        assert w_gate.shape[0] == 2 and mesh.shape["tp"] == 2
        vmem = pl.BlockSpec(memory_space=pltpu.VMEM)
        far = pl.BlockSpec(memory_space=pl.ANY)
        blocks = pltpu.VMEM((2 * n, CAP, half), jnp.bfloat16)
        dma = pltpu.SemaphoreType.DMA
        return pl.pallas_call(
            functools.partial(kernel, n),
            out_shape=jax.ShapeDtypeStruct((rows, half), jnp.bfloat16),
            in_specs=[vmem] * 4 + [far] * 3,
            out_specs=vmem,
            scratch_shapes=[
                pltpu.VMEM((2, 1, half), jnp.float32),
                pltpu.VMEM(w_gate.shape, jnp.bfloat16),
                pltpu.VMEM(w_up.shape, jnp.bfloat16),
                pltpu.VMEM(w_down.shape, jnp.bfloat16),
                blocks, blocks, blocks, blocks,
                dma((3,)), dma((4,)), dma((4,)), dma, dma, dma, dma,
            ],
            compiler_params=pltpu.CompilerParams(collective_id=0, has_side_effects=True),
            name="experts",
        )(tokens, norm_gain.reshape(1, half), routing, route_weight, w_gate, w_up, w_down)

    in_specs = (
        P("ep", "tp"), P("tp"), P("ep", None), P("ep", None),
        P("ep", None, "tp"), P("ep", None, "tp"), P("ep", None, "tp"),
    )
    return jax.shard_map(local, mesh=mesh, in_specs=in_specs, out_specs=P("ep", "tp"), check_vma=False)
```

```python
import functools

import jax
import jax.numpy as jnp
from jax import lax
from jax.experimental import pallas as pl
from jax.experimental.pallas import tpu as pltpu
from jax.sharding import PartitionSpec as P

CAP = 8
EPSILON = 1e-06
MESH = pl.DeviceIdType.MESH


def each(count, body):
    if count <= 16:
        for k in range(1, count):
            body(k)
    else:
        lax.fori_loop(1, count, lambda k, c: (body(k), c)[1], 0)


def kernel(
    n, tok_hbm, gain_hbm, routing_hbm, weight_hbm, wg_hbm, wu_hbm, wd_hbm, out_ref,
    tok, routing, weight, gains, wg, wu, wd, send_x, recv_x, send_y, recv_y,
    in_sem, own_sem, far_send, far_recv, sx_sem, rx_sem, sy_sem, ry_sem,
):
    me, core = lax.axis_index("ep"), lax.axis_index("tp")
    other = 1 - core
    tokens, half = tok.shape
    slots = 2 * n * CAP

    stores = ((wg_hbm, wg), (wu_hbm, wu), (wd_hbm, wd))
    inputs = ((routing_hbm, routing), (tok_hbm, tok), (weight_hbm, weight), (gain_hbm, gains.at[core]))
    inputs = [pltpu.make_async_copy(src, dst, in_sem.at[i]) for i, (src, dst) in enumerate(inputs)]
    own = [
        pltpu.make_async_copy(src.at[core], dst.at[core], own_sem.at[i])
        for i, (src, dst) in enumerate(stores)
    ]
    for copy in inputs:
        copy.start()

    barrier = pltpu.get_barrier_semaphore()

    def greet(k):
        peer = lax.rem(me + k, n)
        for c in range(2):
            pl.semaphore_signal(barrier, inc=1, device_id=(peer, c), device_id_type=MESH)

    each(n, greet)
    pl.semaphore_signal(barrier, inc=1, device_id=(me, other), device_id_type=MESH)
    for copy in own:
        copy.start()

    experts = 2 * n
    names = lax.broadcasted_iota(jnp.int32, (experts, tokens), 0)
    row = lax.broadcasted_iota(jnp.int32, (tokens, tokens), 0)
    col = lax.broadcasted_iota(jnp.int32, (tokens, tokens), 1)
    before = (row < col).astype(jnp.float32).astype(jnp.bfloat16)
    places = lax.broadcasted_iota(jnp.int32, (slots, tokens), 0)
    inputs[0].wait()
    picks = [routing[k:k + 1, :] for k in range(2)]
    hot = [(picks[k] == names).astype(jnp.float32) for k in range(2)]
    earlier = jnp.dot((hot[0] + hot[1]).astype(jnp.bfloat16), before, preferred_element_type=jnp.float32)
    chosen = []
    for k in range(2):
        rank = jnp.sum(earlier * hot[k], axis=0, keepdims=True).astype(jnp.int32)
        chosen.append((places == picks[k] * CAP + rank).astype(jnp.float32))
    spread = (chosen[0] + chosen[1]).astype(jnp.bfloat16)
    inputs[1].wait()
    outgoing = jnp.dot(spread, tok[...], preferred_element_type=jnp.float32)
    send_x[...] = outgoing.reshape(2 * n, CAP, half).astype(jnp.bfloat16)
    pick_rows = [jnp.transpose(c).astype(jnp.bfloat16) for c in chosen]
    inputs[2].wait()
    pick_weight = [jnp.transpose(jnp.broadcast_to(weight[k:k + 1, :], (CAP, tokens)))[:, :1] for k in range(2)]

    pl.semaphore_wait(barrier, 2 * n - 1)
    def remote(src, dst, send, recv, peer, c):
        return pltpu.make_async_remote_copy(
            src_ref=src, dst_ref=dst, send_sem=send, recv_sem=recv,
            device_id=(peer, c), device_id_type=MESH,
        )

    def post(k):
        peer = lax.rem(me + k, n)
        for c in range(2):
            remote(send_x.at[peer * 2 + c], recv_x.at[core * n + me], sx_sem, rx_sem, peer, c).start()

    each(n, post)
    remote(send_x.at[me * 2 + other], recv_x.at[core * n + me], sx_sem, rx_sem, me, other).start()
    pltpu.make_async_copy(send_x.at[me * 2 + core], recv_x.at[core * n + me], rx_sem).start()
    inputs[3].wait()
    far = [remote(gain_hbm, gains.at[core], far_send.at[3], far_recv.at[3], me, other)] + [
        remote(src.at[other], dst.at[core], far_send.at[i], far_recv.at[i], me, other)
        for i, (src, dst) in enumerate(stores)
    ]
    for copy in far:
        copy.start()

    for copy in own:
        copy.wait()
    for copy in far:
        copy.wait()
    pltpu.make_async_copy(recv_x, recv_x, rx_sem).wait()
    sent = pl.ds(0, 2 * n - 1)
    rows = n * CAP
    parts = [recv_x[h * n:(h + 1) * n].astype(jnp.float32).reshape(rows, half) for h in range(2)]
    squares = sum(jnp.sum(p * p, axis=1, keepdims=True) for p in parts)
    scale = lax.rsqrt(squares / (2 * half) + EPSILON)
    normed = jnp.concatenate(
        [(p * scale * gains[h]).astype(jnp.bfloat16) for h, p in enumerate(parts)], axis=1
    )
    hidden = []
    for h in range(2):
        gate = jnp.dot(normed, wg[h], preferred_element_type=jnp.float32)
        up = jnp.dot(normed, wu[h], preferred_element_type=jnp.float32)
        hidden.append((jax.nn.silu(gate) * up).astype(jnp.bfloat16))
    hidden = jnp.concatenate(hidden, axis=1)
    for f in range(2):
        result = jnp.dot(hidden, wd[f], preferred_element_type=jnp.float32)
        send_y[f * n:(f + 1) * n] = result.reshape(n, CAP, half).astype(jnp.bfloat16)
    def reply(k):
        peer = lax.rem(me + k, n)
        for c in range(2):
            remote(send_y.at[c * n + peer], recv_y.at[me * 2 + core], sy_sem, ry_sem, peer, c).start()

    each(n, reply)
    remote(send_y.at[other * n + me], recv_y.at[me * 2 + core], sy_sem, ry_sem, me, other).start()
    pltpu.make_async_copy(send_y.at[core * n + me], recv_y.at[me * 2 + core], ry_sem).start()
    pltpu.make_async_copy(recv_y, recv_y, ry_sem).wait()

    back = recv_y[...].astype(jnp.float32).reshape(slots, half).astype(jnp.bfloat16)
    total = 0.0
    for k in range(2):
        total = total + pick_weight[k] * jnp.dot(pick_rows[k], back, preferred_element_type=jnp.float32)
    out_ref[...] = total.astype(jnp.bfloat16)
    pltpu.make_async_copy(send_x.at[sent], send_x.at[sent], sx_sem).wait()
    pltpu.make_async_copy(send_y.at[sent], send_y.at[sent], sy_sem).wait()


def solution(mesh):
    n = mesh.shape["ep"]

    def local(tokens, norm_gain, routing, route_weight, w_gate, w_up, w_down):
        rows, half = tokens.shape
        assert w_gate.shape[0] == 2 and mesh.shape["tp"] == 2
        vmem = pl.BlockSpec(memory_space=pltpu.VMEM)
        far = pl.BlockSpec(memory_space=pl.ANY)
        blocks = pltpu.VMEM((2 * n, CAP, half), jnp.bfloat16)
        dma = pltpu.SemaphoreType.DMA
        return pl.pallas_call(
            functools.partial(kernel, n),
            out_shape=pltpu.VMEM((rows, half), jnp.bfloat16),
            in_specs=[far] * 7,
            out_specs=vmem,
            scratch_shapes=[
                pltpu.VMEM((rows, half), jnp.bfloat16),
                pltpu.VMEM((2, rows), jnp.int32),
                pltpu.VMEM((2, rows), jnp.float32),
                pltpu.VMEM((2, 1, half), jnp.float32),
                pltpu.VMEM(w_gate.shape, jnp.bfloat16),
                pltpu.VMEM(w_up.shape, jnp.bfloat16),
                pltpu.VMEM(w_down.shape, jnp.bfloat16),
                blocks, blocks, blocks, blocks,
                dma((4,)), dma((3,)), dma((4,)), dma((4,)), dma, dma, dma, dma,
            ],
            compiler_params=pltpu.CompilerParams(collective_id=0, has_side_effects=True),
            name="experts",
        )(tokens, norm_gain.reshape(1, half), routing.T, route_weight.T, w_gate, w_up, w_down)

    in_specs = (
        P("ep", "tp"), P("tp"), P("ep", None), P("ep", None),
        P("ep", None, "tp"), P("ep", None, "tp"), P("ep", None, "tp"),
    )
    return jax.shard_map(local, mesh=mesh, in_specs=in_specs, out_specs=P("ep", "tp"), check_vma=False)
```

```python
import functools

import jax
import jax.numpy as jnp
from jax import lax
from jax.experimental import pallas as pl
from jax.experimental.pallas import tpu as pltpu
from jax.sharding import PartitionSpec as P

CAP = 8
EPSILON = 1e-06
MESH = pl.DeviceIdType.MESH


GROUPS = 4


def each(count, body):
    if count <= 16:
        for j in range(1, count):
            body(j)
    else:
        lax.fori_loop(1, count, lambda j, c: (body(j), c)[1], 0)


def ahead(me, j, n):
    return lax.rem(me + n - j, n)


def behind(me, j, n):
    return lax.rem(me + j, n)


def kernel(
    n, tok_hbm, gain_hbm, routing_hbm, weight_hbm, wg_hbm, wu_hbm, wd_hbm, out_ref,
    tok, routing, weight, gains, wg, wu, wd, give_g, give_u, give_d, send_x, recv_x, send_y, recv_y,
    in_sem, own_sem, give_sem, far_send, far_recv, sx_sem, rx_sem, sy_sem, ry_sem,
):
    me, core = lax.axis_index("ep"), lax.axis_index("tp")
    other = 1 - core
    tokens, half = tok.shape
    slots = 2 * n * CAP
    span = n // GROUPS

    stores = ((wg_hbm, wg, give_g), (wu_hbm, wu, give_u), (wd_hbm, wd, give_d))
    inputs = ((routing_hbm, routing), (tok_hbm, tok), (weight_hbm, weight), (gain_hbm, gains.at[core]))
    inputs = [pltpu.make_async_copy(src, dst, in_sem.at[i]) for i, (src, dst) in enumerate(inputs)]
    own = [
        pltpu.make_async_copy(src.at[core], dst.at[core], own_sem.at[i])
        for i, (src, dst, _) in enumerate(stores)
    ]
    give = [
        pltpu.make_async_copy(src.at[other], stage, give_sem.at[i])
        for i, (src, _, stage) in enumerate(stores)
    ]
    for copy in inputs:
        copy.start()

    barrier = pltpu.get_barrier_semaphore()

    def greet(j):
        peer = ahead(me, j, n)
        for c in range(2):
            pl.semaphore_signal(barrier, inc=1, device_id=(peer, c), device_id_type=MESH)

    each(n, greet)
    pl.semaphore_signal(barrier, inc=1, device_id=(me, other), device_id_type=MESH)
    for copy in give + own:
        copy.start()

    experts = 2 * n
    names = lax.broadcasted_iota(jnp.int32, (experts, tokens), 0)
    row = lax.broadcasted_iota(jnp.int32, (tokens, tokens), 0)
    col = lax.broadcasted_iota(jnp.int32, (tokens, tokens), 1)
    before = (row < col).astype(jnp.float32).astype(jnp.bfloat16)
    places = lax.broadcasted_iota(jnp.int32, (slots, tokens), 0)
    inputs[0].wait()
    picks = [routing[k:k + 1, :] for k in range(2)]
    hot = [(picks[k] == names).astype(jnp.float32) for k in range(2)]
    earlier = jnp.dot((hot[0] + hot[1]).astype(jnp.bfloat16), before, preferred_element_type=jnp.float32)
    chosen = []
    for k in range(2):
        rank = jnp.sum(earlier * hot[k], axis=0, keepdims=True).astype(jnp.int32)
        chosen.append((places == picks[k] * CAP + rank).astype(jnp.float32))
    spread = (chosen[0] + chosen[1]).astype(jnp.bfloat16)
    inputs[1].wait()
    outgoing = jnp.dot(spread, tok[...], preferred_element_type=jnp.float32)
    send_x[...] = outgoing.reshape(2 * n, CAP, half).astype(jnp.bfloat16)
    pick_rows = [jnp.transpose(c).astype(jnp.bfloat16) for c in chosen]
    inputs[2].wait()
    pick_weight = [jnp.transpose(jnp.broadcast_to(weight[k:k + 1, :], (CAP, tokens)))[:, :1] for k in range(2)]
    for copy in inputs[3:] + give:
        copy.wait()

    pl.semaphore_wait(barrier, 2 * n - 1)

    def remote(src, dst, send, recv, peer, c):
        return pltpu.make_async_remote_copy(
            src_ref=src, dst_ref=dst, send_sem=send, recv_sem=recv,
            device_id=(peer, c), device_id_type=MESH,
        )

    def block(j, h):
        return (j // span * 2 + h) * span + j % span

    gain_copy = remote(gains.at[core], gains.at[core], far_send.at[3], far_recv.at[3], me, other)
    gain_copy.start()
    remote(send_x.at[me * 2 + other], recv_x.at[block(0, core)], sx_sem, rx_sem.at[0], me, other).start()
    pltpu.make_async_copy(send_x.at[me * 2 + core], recv_x.at[block(0, core)], rx_sem.at[0]).start()

    def post(j):
        peer = ahead(me, j, n)
        for c in range(2):
            remote(
                send_x.at[peer * 2 + c], recv_x.at[block(j, core)], sx_sem, rx_sem.at[j // span], peer, c
            ).start()

    far = [
        remote(stage, dst.at[core], far_send.at[i], far_recv.at[i], me, other)
        for i, (_, dst, stage) in enumerate(stores)
    ]
    for copy in far:
        copy.start()
    each(n, post)

    for copy in own:
        copy.wait()
    gain_copy.wait()

    def reply(j):
        peer = behind(me, j, n)
        for c in range(2):
            remote(send_y.at[block(j, c)], recv_y.at[me * 2 + core], sy_sem, ry_sem, peer, c).start()

    rows = span * CAP
    for g in range(GROUPS):
        here = recv_x.at[pl.ds(2 * g * span, 2 * span)]
        pltpu.make_async_copy(here, here, rx_sem.at[g]).wait()
        parts = [
            recv_x[(2 * g + h) * span:(2 * g + h + 1) * span].astype(jnp.float32).reshape(rows, half)
            for h in range(2)
        ]
        squares = sum(jnp.sum(p * p, axis=1, keepdims=True) for p in parts)
        scale = lax.rsqrt(squares / (2 * half) + EPSILON)
        normed = jnp.concatenate(
            [(p * scale * gains[h]).astype(jnp.bfloat16) for h, p in enumerate(parts)], axis=1
        )
        if g == 0:
            far[0].wait()
            far[1].wait()
        hidden = []
        for h in range(2):
            gate = jnp.dot(normed, wg[h], preferred_element_type=jnp.float32)
            up = jnp.dot(normed, wu[h], preferred_element_type=jnp.float32)
            hidden.append((jax.nn.silu(gate) * up).astype(jnp.bfloat16))
        hidden = jnp.concatenate(hidden, axis=1)
        if g == 0:
            far[2].wait()
        for f in range(2):
            result = jnp.dot(hidden, wd[f], preferred_element_type=jnp.float32)
            first = (2 * g + f) * span
            send_y[first:first + span] = result.reshape(span, CAP, half).astype(jnp.bfloat16)
        if g == 0:
            remote(send_y.at[block(0, other)], recv_y.at[me * 2 + core], sy_sem, ry_sem, me, other).start()
            pltpu.make_async_copy(send_y.at[block(0, core)], recv_y.at[me * 2 + core], ry_sem).start()
        if span <= 16:
            for j in range(max(g * span, 1), (g + 1) * span):
                reply(j)
        else:
            lax.fori_loop(max(g * span, 1), (g + 1) * span, lambda j, c: (reply(j), c)[1], 0)

    pltpu.make_async_copy(recv_y, recv_y, ry_sem).wait()
    back = recv_y[...].astype(jnp.float32).reshape(slots, half).astype(jnp.bfloat16)
    total = 0.0
    for k in range(2):
        total = total + pick_weight[k] * jnp.dot(pick_rows[k], back, preferred_element_type=jnp.float32)
    out_ref[...] = total.astype(jnp.bfloat16)
    sent = pl.ds(0, 2 * n - 1)
    pltpu.make_async_copy(send_x.at[sent], send_x.at[sent], sx_sem).wait()
    pltpu.make_async_copy(send_y.at[sent], send_y.at[sent], sy_sem).wait()


def solution(mesh):
    n = mesh.shape["ep"]

    def local(tokens, norm_gain, routing, route_weight, w_gate, w_up, w_down):
        rows, half = tokens.shape
        assert w_gate.shape[0] == 2 and mesh.shape["tp"] == 2
        vmem = pl.BlockSpec(memory_space=pltpu.VMEM)
        far = pl.BlockSpec(memory_space=pl.ANY)
        blocks = pltpu.VMEM((2 * n, CAP, half), jnp.bfloat16)
        dma = pltpu.SemaphoreType.DMA
        return pl.pallas_call(
            functools.partial(kernel, n),
            out_shape=pltpu.VMEM((rows, half), jnp.bfloat16),
            in_specs=[far] * 7,
            out_specs=vmem,
            scratch_shapes=[
                pltpu.VMEM((rows, half), jnp.bfloat16),
                pltpu.VMEM((2, rows), jnp.int32),
                pltpu.VMEM((2, rows), jnp.float32),
                pltpu.VMEM((2, 1, half), jnp.float32),
                pltpu.VMEM(w_gate.shape, jnp.bfloat16),
                pltpu.VMEM(w_up.shape, jnp.bfloat16),
                pltpu.VMEM(w_down.shape, jnp.bfloat16),
                pltpu.VMEM(w_gate.shape[1:], jnp.bfloat16),
                pltpu.VMEM(w_up.shape[1:], jnp.bfloat16),
                pltpu.VMEM(w_down.shape[1:], jnp.bfloat16),
                blocks, blocks, blocks, blocks,
                dma((4,)), dma((3,)), dma((3,)), dma((4,)), dma((4,)), dma, dma((GROUPS,)), dma, dma,
            ],
            compiler_params=pltpu.CompilerParams(collective_id=0, has_side_effects=True),
            name="experts",
        )(tokens, norm_gain.reshape(1, half), routing.T, route_weight.T, w_gate, w_up, w_down)

    in_specs = (
        P("ep", "tp"), P("tp"), P("ep", None), P("ep", None),
        P("ep", None, "tp"), P("ep", None, "tp"), P("ep", None, "tp"),
    )
    return jax.shard_map(local, mesh=mesh, in_specs=in_specs, out_specs=P("ep", "tp"), check_vma=False)
```
